512 devices in a mesh: grp: 2 (over y), ep: 32 (over z, core), tp: 8 (over x).
Axes of the slice: x: 8, y: 2, z: 16, core: 2. Of those that a mesh axis runs over, the one named last changes fastest.
The devices are a block of a 8x8x16 slice.
Arguments:
- tokens: bfloat16 [16384, 2048], P(('grp', 'ep'), 'tp'), parts along dimension 0, may hold values from -6 to 6
- norm_gain: float32 [2048], replicated, may hold values from 0.1 to 1.9
- expert_ids: int32 [16384, 2], P(('grp', 'ep')), parts along dimension 0, may hold values from 0 to 31, all different within a row; in each aligned block of 256 rows (0 to 255, 256 to 511, ...) at most 24 rows name the same one
- gate_weights: float32 [16384, 2], P(('grp', 'ep')), parts along dimension 0, may hold values from 0.25 to 1
- w_gate: bfloat16 [32, 2048, 3072], P('ep', None, 'tp'), may hold values from -0.125 to 0.125
- w_up: bfloat16 [32, 2048, 3072], P('ep', None, 'tp'), may hold values from -0.125 to 0.125
- w_down: bfloat16 [32, 3072, 2048], P('ep', 'tp'), may hold values from -0.15625 to 0.15625
Outputs:
- mixed: bfloat16 [16384, 2048], P(('grp', 'ep'), 'tp'), parts along dimension 0
The draws below stay inside these ranges and needn't reach their ends.
There are 2 independent parts, one for each index of `grp`. The reference program is written for one: setup_inputs(seed, part) draws one part's arguments, and reference() takes and returns one part's arrays. A program takes and returns all parts, laid end to end along the dimension named above; an argument that names none is the same for every part. Nothing has to cross between parts.
Inputs may be any that keep to these rules, and one draw needn't show every extreme that they name: `expert_ids`: each token names 2 different experts. Within the 256 rows of one index of ep (aligned blocks) no expert is named more than 24 times, and in some blocks one expert is named exactly 24 times.
All inputs are finite; a program needn't handle non-finite values.
Results may differ from the reference program's by a relative error of at most 0.015.
Values may be sent and summed in bfloat16 or wider, within the bound.
A program may use at most 64 MiB of HBM per device.

```python
import math
import jax
import jax.numpy as jnp
import numpy as np
from jax import lax

D = 2048
FF = 3072
TOP = 2
TOK_DEV = 256
EXPERTS = 32
CAP = 24
TOKENS = 8192
N_EP = 32
N_TP = 8


def with_spikes(result, stream_key, source, target, blocks, factor):
    def block_of(dim):
        return (jnp.arange(result.shape[dim]) // (result.shape[dim] // blocks)).reshape((-1,) + (1,) * (result.ndim - 1 - dim))

    one_side = jax.random.permutation(stream_key, blocks)[block_of(target)]
    other_side = (block_of(target) + blocks // 2) % blocks
    return jnp.where((block_of(source) == one_side) | (block_of(source) == other_side), factor * result, result)


def block_levels(own_key, extent, shards, least, top_value):
    def one(dim, parts):
        steps = jax.random.uniform(jax.random.fold_in(jax.random.fold_in(own_key, 6), dim), (parts,), jnp.float32, least / len(shards), top_value / len(shards))
        return jnp.repeat(jnp.exp(steps), extent[dim] // parts).reshape((-1,) + (1,) * (len(extent) - dim - 1))

    level = one(*shards[0])
    for cut in shards[1:]:
        level = level * one(*cut)
    return level


def deal_out(key, own, number, rows, amount, top, reach, slope):
    ranking = jax.random.permutation(key, amount)
    packed, ordinary = shares(amount, rows * top, reach, slope, True), shares(amount, rows * top, reach, slope, False)
    places = jnp.arange(amount)

    def named(lengths, turn):
        used = int((lengths > 0).sum())
        fixed = max(1, used // 4)
        passed = fixed + (places - fixed + turn * (used - fixed)) % max(1, amount - fixed)
        return jnp.zeros((amount,), jnp.int32).at[ranking[jnp.where(places < fixed, places, passed)]].set(jnp.asarray(lengths, jnp.int32))

    lengths = jnp.where(number % 4 == 0, named(packed, number // 4), named(ordinary, number - number // 4 - 1))
    mixed = jax.random.permutation(jax.random.fold_in(own, 3), amount)
    donor, receiver = mixed[0:amount // 2 * 2:2], mixed[1:amount // 2 * 2:2]
    slack = jnp.minimum(lengths[donor] - 1, reach - lengths[receiver]) // 2
    slack = jnp.where((donor == ranking[0]) | (receiver == ranking[0]) | (lengths[receiver] == 0), 0, jnp.maximum(slack, 0))
    passed = jax.random.randint(jax.random.fold_in(own, 4), (amount // 2,), 0, 1 << 20) % (slack + 1)
    lengths = lengths.at[donor].add(-passed).at[receiver].add(passed)
    members = jnp.searchsorted(jnp.cumsum(lengths), jnp.arange(rows * top), side="right").astype(jnp.int32)
    listing = members.reshape(top, rows).T
    listing = listing[jax.random.permutation(jax.random.fold_in(own, 1), rows)]
    turn = jax.random.randint(jax.random.fold_in(own, 2), (rows, 1), 0, top)
    return jnp.take_along_axis(listing, (jnp.arange(top)[None, :] + turn) % top, axis=1)


def shares(number_of, total, bound, skew, full):
    portions = [(1 << 20) // math.isqrt(rank ** skew) + 1 for rank in range(1, number_of + 1)]
    largest = bound if full else min(bound, max(-(-total // number_of), total * portions[0] // sum(portions)))
    least = 1 if total - largest >= number_of - 1 else 0
    given, spare = [largest] + [least] * (number_of - 1), total - largest - least * (number_of - 1)
    while spare > 0:
        free = [i for i in range(1, number_of) if given[i] < largest] or [i for i in range(1, number_of) if given[i] < bound]
        pool, budget = sum([portions[i] for i in free]), spare
        for i in free:
            extra = min(bound - given[i], max(1, budget * portions[i] // pool), spare)
            given[i] = given[i] + extra
            spare = spare - extra
    return np.array(given)


def gaussian(key, dims, spread, bound, split=(), kind=jnp.bfloat16):
    array = jax.random.normal(key, dims, jnp.float32) * spread
    if len(split) > 0:
        array = block_levels(key, dims, split, -0.22, 0.18) * array
    return jnp.clip(array, min=-bound, max=bound).astype(kind)


def heavy_noise(key, shape, spread, most, shards, heavy, kind=jnp.bfloat16):
    values = spread * jax.random.normal(key, shape, jnp.float32)
    if shards:
        values = values * block_levels(key, shape, shards, -0.22, 0.18)
    return jnp.clip(with_spikes(values, jax.random.fold_in(key, 3), *heavy), -most, most).astype(kind)


def setup_inputs(seed: int = 0, part: int = 0) -> dict:
    seeds = jax.random.split(jax.random.key(seed), 8)
    own_keys = jax.random.split(jax.random.fold_in(seeds[7], part), 8)
    tokens = gaussian(own_keys[0], (TOKENS, D), 1.0, 6.0, ((0, 32), (1, 8)))
    norm_gain = jnp.clip(1.0 + 0.18 * jax.random.normal(seeds[1], (D,), jnp.float32), 0.1, 1.9)
    expert_ids_keys = jax.random.split(jax.random.fold_in(own_keys[2], 1), TOKENS // TOK_DEV)
    expert_ids_turns = jax.random.permutation(jax.random.fold_in(own_keys[2], 3), TOKENS // TOK_DEV)
    expert_ids = jax.vmap(lambda own, number: deal_out(jax.random.fold_in(own_keys[2], 2), own, number, TOK_DEV, EXPERTS, TOP, CAP, 2))(expert_ids_keys, expert_ids_turns).reshape((TOKENS, TOP))
    gate_weights = jnp.clip(0.25 + 0.75 * jax.random.uniform(own_keys[3], (TOKENS, TOP), jnp.float32) ** block_levels(own_keys[3], (TOKENS, TOP), ((0, 32),), -0.2, 0.2), 0.25, 1.0)
    w_gate = gaussian(seeds[4], (EXPERTS, D, FF), D ** -0.5, 0.125, ((0, 32), (2, 8)))
    w_up = gaussian(seeds[5], (EXPERTS, D, FF), D ** -0.5, 0.125, ((0, 32), (2, 8)))
    w_down = heavy_noise(seeds[6], (EXPERTS, FF, D), FF ** -0.5, 0.15625, ((0, 32), (1, 8)), (1, 2, 8, 2.0))
    return dict(tokens=tokens, norm_gain=norm_gain, expert_ids=expert_ids, gate_weights=gate_weights, w_gate=w_gate, w_up=w_up, w_down=w_down)


epsilon = 1e-06

def reference(tokens, norm_gain, expert_ids, gate_weights, w_gate, w_up, w_down):
    tok_values = tokens.astype(jnp.float32)
    mean_square = lax.optimization_barrier(jnp.mean(tok_values * tok_values, axis=1, keepdims=True))
    normed = (tok_values * lax.rsqrt(mean_square + epsilon) * norm_gain.astype(jnp.float32)).astype(jnp.bfloat16)
    assign_count = TOK_DEV * TOP
    block_ids = expert_ids.reshape(N_EP, assign_count)
    onehot = (block_ids[:, :, None] == jnp.arange(EXPERTS, dtype=jnp.int32)[None, None, :]).astype(jnp.int32)
    earlier = jnp.cumsum(onehot, axis=1) - onehot
    slot_index = lax.optimization_barrier(jnp.sum(earlier * onehot, axis=2)).astype(jnp.int32)
    block_index = jnp.arange(N_EP, dtype=jnp.int32)[:, None]
    dest_index = ((block_ids * N_EP + block_index) * CAP + slot_index).astype(jnp.int32)
    owner_index = (block_index * TOK_DEV + jnp.arange(assign_count, dtype=jnp.int32)[None, :] // TOP).astype(jnp.int32)
    slot_token = jnp.full((EXPERTS * N_EP * CAP,), TOKENS, jnp.int32)
    slot_token = slot_token.at[dest_index.reshape(-1)].set(owner_index.reshape(-1))
    slot_token = slot_token.reshape(EXPERTS, N_EP * CAP)

    def run_expert(inputs):
        token_list, gate_matrix, up_matrix, down_matrix = inputs
        tok_rows = jnp.take(normed, token_list, axis=0, mode='fill', fill_value=0)
        gate_part = jnp.dot(tok_rows, gate_matrix, preferred_element_type=jnp.float32)
        up_part = jnp.dot(tok_rows, up_matrix, preferred_element_type=jnp.float32)
        hidden = (jax.nn.silu(gate_part) * up_part).astype(jnp.bfloat16)
        hidden_blocks = hidden.reshape(-1, N_TP, FF // N_TP).astype(jnp.float32)
        down_blocks = down_matrix.reshape(N_TP, FF // N_TP, D).astype(jnp.float32)
        partial_value = jnp.einsum('mtf,tfd->tmd', hidden_blocks, down_blocks).astype(jnp.bfloat16)
        partial_value = lax.optimization_barrier(partial_value)
        return lax.optimization_barrier(jnp.sum(partial_value.astype(jnp.float32), axis=0)).astype(jnp.bfloat16)
    expert_out = lax.map(run_expert, (slot_token, w_gate, w_up, w_down))
    picked = expert_out.reshape(-1, D)[dest_index.reshape(-1)].astype(jnp.float32)
    weighted = picked * gate_weights.reshape(-1)[:, None].astype(jnp.float32)
    return lax.optimization_barrier(jnp.sum(weighted.reshape(TOKENS, TOP, D), axis=1)).astype(jnp.bfloat16)
```

```python
import functools

import jax
import jax.numpy as jnp
from jax import lax
from jax.experimental import pallas as pl
from jax.experimental.pallas import tpu as pltpu
from jax.sharding import PartitionSpec as P

MESH = pl.DeviceIdType.MESH
F32 = jnp.float32
BF16 = jnp.bfloat16
EPS = 1e-06
SLOTS = 4


def dot_nn(a, b):
    return jnp.dot(a, b, preferred_element_type=F32)


def dot_nt(a, b):
    return lax.dot_general(a, b, (((1,), (1,)), ((), ())), preferred_element_type=F32)


def stacked(y):
    rows = y.shape[0]
    left = y[:, :128].reshape(rows // 8, 1, 8, 128)
    right = y[:, 128:].reshape(rows // 8, 1, 8, 128)
    return jnp.concatenate([left, right], axis=1).reshape(2 * rows, 128)


def kernel(
    n_ep, n_tp, cap,
    tok_ref, gain_ref, ids_ref, gw_ref, wg_ref, wu_ref, wd_ref,
    out_ref,
    wgu, wdn, sbuf, xg, lhs, part, stage, rs, yout, back, wt,
    w_sem, z_send, z_recv, ag_send, ag_recv, rs_send, rs_recv, ret_send, ret_recv,
):
    n_z = n_ep // 2
    hops = n_tp // 2
    chunks = n_ep // SLOTS
    tok_count, feats = tok_ref.shape
    ff = wg_ref.shape[1]
    width = feats * n_tp
    rows = SLOTS * cap
    rows2 = 2 * rows
    half = SLOTS // 2
    me = lax.axis_index("ep")
    mt = lax.axis_index("tp")
    z, core = me // 2, me % 2
    SGN = (1, -1)

    loads = [
        pltpu.make_async_copy(wg_ref, wgu.at[:, pl.ds(0, ff)], w_sem.at[0]),
        pltpu.make_async_copy(wu_ref, wgu.at[:, pl.ds(ff, ff)], w_sem.at[1]),
        pltpu.make_async_copy(wd_ref, wdn, w_sem.at[2]),
    ]
    for load in loads:
        load.start()

    barrier = pltpu.get_barrier_semaphore()

    @pl.loop(1, n_ep)
    def _(d):
        pl.semaphore_signal(
            barrier, inc=1, device_id={"ep": (me + d) % n_ep}, device_id_type=MESH
        )

    for sg in SGN:
        pl.semaphore_signal(
            barrier, inc=1, device_id={"tp": (mt + sg + n_tp) % n_tp}, device_id_type=MESH
        )

    e_iota = lax.broadcasted_iota(jnp.int32, (n_ep, tok_count), 0)
    m0 = ids_ref[0:1, :] == e_iota
    m1 = ids_ref[1:2, :] == e_iota
    member = jnp.where(m0 | m1, 1.0, 0.0).astype(F32)
    member_b = member.astype(BF16)
    t_row = lax.broadcasted_iota(jnp.int32, (tok_count, tok_count), 0)
    t_col = lax.broadcasted_iota(jnp.int32, (tok_count, tok_count), 1)
    upper = jnp.where(t_row < t_col, 1.0, 0.0).astype(BF16)
    rank = dot_nn(member_b, upper)
    rank = jnp.where(member > 0.5, rank, -1.0).astype(BF16)
    expand = (
        lax.broadcasted_iota(jnp.int32, (n_ep, cap, n_ep), 0)
        == lax.broadcasted_iota(jnp.int32, (n_ep, cap, n_ep), 2)
    )
    expand = jnp.where(expand, 1.0, 0.0).astype(F32).reshape(n_ep * cap, n_ep).astype(BF16)
    c_iota = lax.broadcasted_iota(jnp.int32, (n_ep, cap, tok_count), 1).astype(F32)
    c_iota = c_iota.reshape(n_ep * cap, tok_count)
    pick = jnp.where(dot_nn(expand, rank) == c_iota, 1.0, 0.0).astype(BF16)
    sent = stacked(dot_nn(pick, tok_ref[...])).astype(BF16)
    sbuf[...] = sent.reshape(n_ep, 2 * cap, 128)
    xg[mt, 0] = sbuf[me]

    def offset(i):
        if n_z >= 8:
            near, tail = 3, 4
            i = i + tail * ((i + n_z - near) // n_z) - (n_z - near) * ((i + tail) // n_z)
        return ((i + 1) // 2) * (2 * (i % 2) - 1)

    def peer(j, sign):
        zz = (z + sign * offset(j // 2) + n_z) % n_z
        return zz * 2 + (core + j % 2) % 2

    def z_copy(j):
        to = peer(j, -1)
        return pltpu.make_async_remote_copy(
            src_ref=sbuf.at[to], dst_ref=xg.at[mt, j],
            send_sem=z_send.at[j], recv_sem=z_recv.at[j],
            device_id={"ep": to}, device_id_type=MESH,
        )

    def ret_copy(j):
        to = peer(j, 1)
        return pltpu.make_async_remote_copy(
            src_ref=yout.at[j], dst_ref=back.at[me],
            send_sem=ret_send.at[j], recv_sem=ret_recv.at[me],
            device_id={"ep": to}, device_id_type=MESH,
        )

    def ret_wait(e):
        pltpu.make_async_remote_copy(
            src_ref=yout.at[0], dst_ref=back.at[e],
            send_sem=ret_send.at[0], recv_sem=ret_recv.at[e],
            device_id={"ep": me}, device_id_type=MESH,
        ).wait_recv()

    def ag_copy(d, s, c, block):
        start = c * SLOTS
        count = SLOTS
        if s == hops - 1:
            start = start + (0 if d == 0 else half)
            count = half
        ref = xg.at[block, pl.ds(start, count)]
        return pltpu.make_async_remote_copy(
            src_ref=ref, dst_ref=ref,
            send_sem=ag_send.at[d, s, c], recv_sem=ag_recv.at[d, s, c],
            device_id={"tp": (mt + SGN[d] + n_tp) % n_tp}, device_id_type=MESH,
        )

    def ag_start(d, s, c):
        ag_copy(d, s, c, (mt - SGN[d] * s + n_tp) % n_tp).start()

    def ag_wait(d, s, c):
        ag_copy(d, s, c, (mt - SGN[d] * (s + 1) + n_tp) % n_tp).wait_recv()

    def rs_copy(d, r, c):
        if r == 0:
            span = pl.ds(0 if d == 0 else rows, rows)
            src, dst = stage.at[d, r, c, span], rs.at[d, r, c, span]
        else:
            src, dst = stage.at[d, r, c], rs.at[d, r, c]
        return pltpu.make_async_remote_copy(
            src_ref=src, dst_ref=dst,
            send_sem=rs_send.at[d, r, c], recv_sem=rs_recv.at[d, r, c],
            device_id={"tp": (mt + SGN[d] + n_tp) % n_tp}, device_id_type=MESH,
        )

    pl.semaphore_wait(barrier, n_ep - 1 + 2)

    @pl.loop(1, n_ep)
    def _(j):
        z_copy(j).start()

    eye = jnp.where(t_row == t_col, 1.0, 0.0).astype(BF16)
    lower = jnp.where(t_col < t_row, 1.0, 0.0).astype(BF16)
    gate_w = jnp.where(m0, gw_ref[0:1, :], 0.0) + jnp.where(m1, gw_ref[1:2, :], 0.0)
    gate_hi = gate_w.astype(BF16)
    gate_lo = (gate_w - gate_hi.astype(F32)).astype(BF16)
    rank_t = jnp.where(dot_nt(eye, member_b) > 0.5, dot_nt(lower, member_b), -1.0).astype(BF16)
    l_e = lax.broadcasted_iota(jnp.int32, (n_ep, n_ep * cap), 0) * cap
    l_s = lax.broadcasted_iota(jnp.int32, (n_ep, n_ep * cap), 1)
    expand_t = jnp.where((l_s >= l_e) & (l_s < l_e + cap), 1.0, 0.0).astype(BF16)
    lane = lax.broadcasted_iota(jnp.int32, (tok_count, n_ep * cap), 1).astype(F32)
    lane_c = lane - cap * jnp.floor((lane + 0.5) * (1.0 / cap))
    hit = dot_nn(rank_t, expand_t) == lane_c
    wt[0] = jnp.where(
        hit, dot_nn(dot_nt(eye, gate_hi).astype(BF16), expand_t), 0.0
    ).astype(BF16)
    wt[1] = jnp.where(
        hit, dot_nn(dot_nt(eye, gate_lo).astype(BF16), expand_t), 0.0
    ).astype(BF16)

    for load in loads:
        load.wait()

    def compute(c):
        total = jnp.zeros((rows // 8, 8, 128), F32)
        for b in range(n_tp):
            v = xg[b, pl.ds(c * SLOTS, SLOTS)].reshape(rows2, 128).astype(F32)
            v = v.reshape(rows // 8, 2, 8, 128)
            for h in range(2):
                vh = v[:, h]
                total = total + vh * vh
                k = 2 * b + h
                scaled = vh * gain_ref[k : k + 1, :].reshape(1, 1, 128)
                lhs[:, k * 128 : (k + 1) * 128] = scaled.reshape(rows, 128).astype(BF16)
        square = jnp.sum(total.reshape(rows, 128), axis=1, keepdims=True)
        scale = lax.rsqrt(square / width + EPS)
        gu = dot_nn(lhs[...], wgu[...])
        gate = gu[:, :ff] * scale
        up = gu[:, ff:] * scale
        hidden = (gate / (1.0 + jnp.exp(-gate)) * up).astype(BF16)
        y = dot_nn(hidden, wdn[...])
        for b in range(n_tp):
            part[c, b] = stacked(y[:, b * feats : (b + 1) * feats])

    def in_range(c):
        return (c >= 0) & (c < chunks)

    @pl.loop(0, chunks + 2 * hops)
    def _(t):
        for s in range(hops - 1, 0, -1):

            @pl.when(in_range(t - s))
            def _():
                c = t - s
                for d in range(2):
                    ag_wait(d, s - 1, c)
                    ag_start(d, s, c)

        @pl.when(t < chunks)
        def _():
            for k in range(SLOTS):
                j = t * SLOTS + k

                def arrived():
                    pltpu.make_async_remote_copy(
                        src_ref=sbuf.at[0], dst_ref=xg.at[mt, j],
                        send_sem=z_send.at[j], recv_sem=z_recv.at[j],
                        device_id={"ep": me}, device_id_type=MESH,
                    ).wait_recv()

                if k == 0:
                    pl.when(t > 0)(arrived)
                else:
                    arrived()
            for d in range(2):
                ag_start(d, 0, t)

        @pl.when(in_range(t - hops))
        def _():
            c = t - hops
            for d in range(2):
                ag_wait(d, hops - 1, c)
            compute(c)

        for r in range(hops - 1, -1, -1):

            @pl.when(in_range(t - hops - r))
            def _():
                c = t - hops - r
                for d in range(2):
                    block = (mt + SGN[d] * (hops - r) + n_tp) % n_tp
                    own = slice(0, rows) if d == 0 else slice(rows, rows2)
                    rest = slice(rows, rows2) if d == 0 else slice(0, rows)
                    if r == 0:
                        stage[d, r, c, own] = part[c, block, own].astype(BF16)
                    elif r == 1:
                        rs_copy(d, 0, c).wait_recv()
                        stage[d, r, c, own] = (
                            part[c, block, own] + rs[d, 0, c, own].astype(F32)
                        ).astype(BF16)
                        stage[d, r, c, rest] = part[c, block, rest].astype(BF16)
                    else:
                        rs_copy(d, r - 1, c).wait_recv()
                        stage[d, r, c] = (
                            part[c, block] + rs[d, r - 1, c].astype(F32)
                        ).astype(BF16)
                    rs_copy(d, r, c).start()

        @pl.when(in_range(t - 2 * hops))
        def _():
            c = t - 2 * hops
            for d in range(2):
                rs_copy(d, hops - 1, c).wait_recv()
            y = (
                part[c, mt]
                + rs[0, hops - 1, c].astype(F32)
                + rs[1, hops - 1, c].astype(F32)
            ).astype(BF16)
            yout[pl.ds(c * SLOTS, SLOTS)] = y.reshape(SLOTS, 2 * cap, 128)
            for k in range(SLOTS):
                j = c * SLOTS + k
                if k == 0:

                    @pl.when(c > 0)
                    def _():
                        ret_copy(j).start()
                else:
                    ret_copy(j).start()

    back[me] = yout[0]

    @pl.loop(1, n_ep)
    def _(d):
        ret_wait((me + d) % n_ep)

    b4 = back[...].reshape(2 * n_ep * cap, 128).astype(F32)
    b4 = b4.reshape(n_ep * cap // 8, 2, 8, 128)
    left = b4[:, 0].reshape(n_ep * cap, 128).astype(BF16)
    right = b4[:, 1].reshape(n_ep * cap, 128).astype(BF16)
    picked = jnp.concatenate([left, right], axis=1)
    out_ref[...] = (dot_nn(wt[0], picked) + dot_nn(wt[1], picked)).astype(BF16)

    @pl.loop(1, n_ep)
    def _(j):
        z_copy(j).wait_send()
        ret_copy(j).wait_send()

    @pl.loop(0, chunks)
    def _(c):
        for d in range(2):
            for s in range(hops):
                ag_copy(d, s, c, mt).wait_send()
                rs_copy(d, s, c).wait_send()


def on_device(n_ep, n_tp, tokens, norm_gain, expert_ids, gate_weights, w_gate, w_up, w_down):
    tok_count, feats = tokens.shape
    cap = 3 * tok_count * expert_ids.shape[1] // (2 * n_ep)
    width, ff = w_gate.shape[1:]
    chunks, hops = n_ep // SLOTS, n_tp // 2
    rows = SLOTS * cap
    vmem = pl.BlockSpec(memory_space=pltpu.VMEM)
    hbm = pl.BlockSpec(memory_space=pl.ANY)
    dma = pltpu.SemaphoreType.DMA
    block = (n_ep, 2 * cap, 128)
    return pl.pallas_call(
        functools.partial(kernel, n_ep, n_tp, cap),
        out_shape=jax.ShapeDtypeStruct((tok_count, feats), BF16),
        in_specs=[vmem, vmem, vmem, vmem, hbm, hbm, hbm],
        out_specs=vmem,
        scratch_shapes=[
            pltpu.VMEM((width, 2 * ff), BF16),
            pltpu.VMEM((ff, width), BF16),
            pltpu.VMEM(block, BF16),
            pltpu.VMEM((n_tp, *block), BF16),
            pltpu.VMEM((rows, width), BF16),
            pltpu.VMEM((chunks, n_tp, 2 * rows, 128), F32),
            pltpu.VMEM((2, hops, chunks, 2 * rows, 128), BF16),
            pltpu.VMEM((2, hops, chunks, 2 * rows, 128), BF16),
            pltpu.VMEM(block, BF16),
            pltpu.VMEM(block, BF16),
            pltpu.VMEM((2, tok_count, n_ep * cap), BF16),
            dma((3,)),
            dma((n_ep,)),
            dma((n_ep,)),
            dma((2, hops, chunks)),
            dma((2, hops, chunks)),
            dma((2, hops, chunks)),
            dma((2, hops, chunks)),
            dma((n_ep,)),
            dma((n_ep,)),
        ],
        compiler_params=pltpu.CompilerParams(
            collective_id=0, has_side_effects=True, vmem_limit_bytes=48 * 1024 * 1024
        ),
    )(
        tokens,
        norm_gain.reshape(-1, 128),
        expert_ids.T,
        gate_weights.T,
        w_gate[0],
        w_up[0],
        w_down[0],
    )


def solution(mesh):
    rows = ("grp", "ep")
    return jax.shard_map(
        functools.partial(on_device, mesh.shape["ep"], mesh.shape["tp"]),
        mesh=mesh,
        in_specs=(
            P(rows, "tp"),
            P(),
            P(rows, None),
            P(rows, None),
            P("ep", None, "tp"),
            P("ep", None, "tp"),
            P("ep", "tp", None),
        ),
        out_specs=P(rows, "tp"),
        check_vma=False,
    )
```

```python
import functools

import jax
import jax.numpy as jnp
from jax import lax
from jax.experimental import pallas as pl
from jax.experimental.pallas import tpu as pltpu
from jax.sharding import PartitionSpec as P

MESH = pl.DeviceIdType.MESH
F32 = jnp.float32
BF16 = jnp.bfloat16
EPS = 1e-06
SLOTS = 4
GROUP = 2
STEPS = (0, 1, 4, -4, 5, -5, 6, -6, 7, -7, 8, 3, -3, 2, -2, -1)


def steps_of(n_z):
    if n_z == len(STEPS):
        return list(STEPS)
    return [0] + [(i + 1) // 2 * (1 if i % 2 else -1) for i in range(1, n_z)]


def dot_nn(a, b):
    return jnp.dot(a, b, preferred_element_type=F32)


def dot_nt(a, b):
    return lax.dot_general(a, b, (((1,), (1,)), ((), ())), preferred_element_type=F32)


def stacked(y):
    rows = y.shape[0]
    left = y[:, :128].reshape(rows // 8, 1, 8, 128)
    right = y[:, 128:].reshape(rows // 8, 1, 8, 128)
    return jnp.concatenate([left, right], axis=1).reshape(2 * rows, 128)


def kernel(
    n_ep, n_tp, cap,
    tok_hbm, gain_hbm, ids_hbm, gw_hbm, wg_ref, wu_ref, wd_ref,
    out_ref,
    tok_ref, gain_ref, ids_ref, gw_ref,
    wgu, wdn, sbuf, xg, lhs, part, stage, rs, yout, back, wt,
    in_sem, w_sem, z_send, z_recv, ag_send, ag_recv, rs_send, rs_recv, ret_send, ret_recv,
):
    n_z = n_ep // 2
    hops = n_tp // 2
    chunks = n_ep // SLOTS
    groups = chunks // GROUP
    wide = GROUP * SLOTS
    tok_count, feats = tok_ref.shape
    ff = wg_ref.shape[1]
    width = feats * n_tp
    rows = SLOTS * cap
    rows2 = 2 * rows
    grows = wide * cap
    half = SLOTS // 2
    me = lax.axis_index("ep")
    mt = lax.axis_index("tp")
    z, core = me // 2, me % 2
    SGN = (1, -1)

    ins = [
        pltpu.make_async_copy(ids_hbm, ids_ref, in_sem.at[0]),
        pltpu.make_async_copy(tok_hbm, tok_ref, in_sem.at[1]),
        pltpu.make_async_copy(gw_hbm, gw_ref, in_sem.at[2]),
        pltpu.make_async_copy(gain_hbm, gain_ref, in_sem.at[3]),
    ]
    for load in ins:
        load.start()

    barrier = pltpu.get_barrier_semaphore()

    @pl.loop(1, n_ep)
    def _(d):
        pl.semaphore_signal(
            barrier, inc=1, device_id={"ep": (me + d) % n_ep}, device_id_type=MESH
        )

    for sg in SGN:
        pl.semaphore_signal(
            barrier, inc=1, device_id={"tp": (mt + sg + n_tp) % n_tp}, device_id_type=MESH
        )

    loads = [
        pltpu.make_async_copy(wg_ref, wgu.at[:, pl.ds(0, ff)], w_sem.at[0]),
        pltpu.make_async_copy(wu_ref, wgu.at[:, pl.ds(ff, ff)], w_sem.at[1]),
        pltpu.make_async_copy(wd_ref, wdn, w_sem.at[2]),
    ]
    for load in loads:
        load.start()

    steps = steps_of(n_z)

    def peer(j, sign):
        zz = (z + sign * steps[j // 2] + n_z) % n_z
        return zz * 2 + (core + j % 2) % 2

    for load in ins:
        load.wait()
    j_iota = lax.broadcasted_iota(jnp.int32, (n_ep, 1), 0)
    e_iota = jnp.zeros((n_ep, 1), jnp.int32)
    for j in range(n_ep):
        e_iota = jnp.where(j_iota == j, peer(j, -1), e_iota)
    m0 = ids_ref[0:1, :] == e_iota
    m1 = ids_ref[1:2, :] == e_iota
    member = jnp.where(m0 | m1, 1.0, 0.0).astype(F32)
    member_b = member.astype(BF16)
    t_row = lax.broadcasted_iota(jnp.int32, (tok_count, tok_count), 0)
    t_col = lax.broadcasted_iota(jnp.int32, (tok_count, tok_count), 1)
    upper = jnp.where(t_row < t_col, 1.0, 0.0).astype(BF16)
    rank = dot_nn(member_b, upper)
    rank = jnp.where(member > 0.5, rank, -1.0).astype(BF16)
    x_row = lax.broadcasted_iota(jnp.int32, (wide, cap, n_ep), 0)
    x_col = lax.broadcasted_iota(jnp.int32, (wide, cap, n_ep), 2)
    c_iota = lax.broadcasted_iota(jnp.int32, (wide, cap, tok_count), 1).astype(F32)
    c_iota = c_iota.reshape(grows, tok_count)

    def z_copy(j):
        return pltpu.make_async_remote_copy(
            src_ref=sbuf.at[j], dst_ref=xg.at[mt, j],
            send_sem=z_send.at[j], recv_sem=z_recv.at[j],
            device_id={"ep": peer(j, -1)}, device_id_type=MESH,
        )

    def ret_copy(j):
        return pltpu.make_async_remote_copy(
            src_ref=yout.at[j], dst_ref=back.at[j],
            send_sem=ret_send.at[j], recv_sem=ret_recv.at[j],
            device_id={"ep": peer(j, 1)}, device_id_type=MESH,
        )

    for g in range(groups):
        expand = jnp.where(x_row + g * wide == x_col, 1.0, 0.0).astype(F32)
        expand = expand.reshape(grows, n_ep).astype(BF16)
        pick = jnp.where(dot_nn(expand, rank) == c_iota, 1.0, 0.0).astype(BF16)
        sent = stacked(dot_nn(pick, tok_ref[...])).astype(BF16)
        sbuf[g * wide : (g + 1) * wide] = sent.reshape(wide, 2 * cap, 128)
        if g == 0:
            xg[mt, 0] = sbuf[0]
            pl.semaphore_wait(barrier, n_ep - 1 + 2)

        for j in range(max(1, g * wide), (g + 1) * wide):
            z_copy(j).start()

    def ag_copy(d, s, c, block):
        start = c * SLOTS
        count = SLOTS
        if s == hops - 1:
            start = start + (0 if d == 0 else half)
            count = half
        ref = xg.at[block, pl.ds(start, count)]
        return pltpu.make_async_remote_copy(
            src_ref=ref, dst_ref=ref,
            send_sem=ag_send.at[d, s, c], recv_sem=ag_recv.at[d, s, c],
            device_id={"tp": (mt + SGN[d] + n_tp) % n_tp}, device_id_type=MESH,
        )

    def ag_start(d, s, c):
        ag_copy(d, s, c, (mt - SGN[d] * s + n_tp) % n_tp).start()

    def ag_wait(d, s, c):
        ag_copy(d, s, c, (mt - SGN[d] * (s + 1) + n_tp) % n_tp).wait_recv()

    def rs_copy(d, r, c):
        if r == 0:
            span = pl.ds(0 if d == 0 else rows, rows)
            src, dst = stage.at[d, r, c, span], rs.at[d, r, c, span]
        else:
            src, dst = stage.at[d, r, c], rs.at[d, r, c]
        return pltpu.make_async_remote_copy(
            src_ref=src, dst_ref=dst,
            send_sem=rs_send.at[d, r, c], recv_sem=rs_recv.at[d, r, c],
            device_id={"tp": (mt + SGN[d] + n_tp) % n_tp}, device_id_type=MESH,
        )

    def combine_weights():
        eye = jnp.where(t_row == t_col, 1.0, 0.0).astype(BF16)
        lower = jnp.where(t_col < t_row, 1.0, 0.0).astype(BF16)
        gate_w = jnp.where(m0, gw_ref[0:1, :], 0.0) + jnp.where(m1, gw_ref[1:2, :], 0.0)
        gate_hi = gate_w.astype(BF16)
        gate_lo = (gate_w - gate_hi.astype(F32)).astype(BF16)
        rank_t = jnp.where(dot_nt(eye, member_b) > 0.5, dot_nt(lower, member_b), -1.0)
        rank_t = rank_t.astype(BF16)
        hi_t = dot_nt(eye, gate_hi).astype(BF16)
        lo_t = dot_nt(eye, gate_lo).astype(BF16)
        l_e = lax.broadcasted_iota(jnp.int32, (n_ep, grows), 0) * cap
        l_s = lax.broadcasted_iota(jnp.int32, (n_ep, grows), 1)
        lane = lax.broadcasted_iota(jnp.int32, (tok_count, grows), 1).astype(F32)
        lane = lane - cap * jnp.floor((lane + 0.5) * (1.0 / cap))
        for g in range(groups):
            s = l_s + g * grows
            expand_t = jnp.where((s >= l_e) & (s < l_e + cap), 1.0, 0.0).astype(BF16)
            hit = dot_nn(rank_t, expand_t) == lane
            wt[g, 0] = jnp.where(hit, dot_nn(hi_t, expand_t), 0.0).astype(BF16)
            wt[g, 1] = jnp.where(hit, dot_nn(lo_t, expand_t), 0.0).astype(BF16)

    def compute(c):
        total = jnp.zeros((rows // 8, 8, 128), F32)
        for b in range(n_tp):
            v = xg[b, pl.ds(c * SLOTS, SLOTS)].reshape(rows2, 128).astype(F32)
            v = v.reshape(rows // 8, 2, 8, 128)
            for h in range(2):
                vh = v[:, h]
                total = total + vh * vh
                k = 2 * b + h
                scaled = vh * gain_ref[k : k + 1, :].reshape(1, 1, 128)
                lhs[:, k * 128 : (k + 1) * 128] = scaled.reshape(rows, 128).astype(BF16)
        square = jnp.sum(total.reshape(rows, 128), axis=1, keepdims=True)
        scale = lax.rsqrt(square / width + EPS)
        gu = dot_nn(lhs[...], wgu[...])
        gate = gu[:, :ff] * scale
        up = gu[:, ff:] * scale
        hidden = (gate / (1.0 + jnp.exp(-gate)) * up).astype(BF16)
        y = dot_nn(hidden, wdn[...])
        for b in range(n_tp):
            part[c, b] = stacked(y[:, b * feats : (b + 1) * feats])

    def reduce_step(d, r, c):
        block = (mt + SGN[d] * (hops - r) + n_tp) % n_tp
        own = slice(0, rows) if d == 0 else slice(rows, rows2)
        rest = slice(rows, rows2) if d == 0 else slice(0, rows)
        if r == 0:
            stage[d, r, c, own] = part[c, block, own].astype(BF16)
        elif r == 1:
            rs_copy(d, 0, c).wait_recv()
            stage[d, r, c, own] = (
                part[c, block, own] + rs[d, 0, c, own].astype(F32)
            ).astype(BF16)
            stage[d, r, c, rest] = part[c, block, rest].astype(BF16)
        else:
            rs_copy(d, r - 1, c).wait_recv()
            stage[d, r, c] = (part[c, block] + rs[d, r - 1, c].astype(F32)).astype(BF16)
        rs_copy(d, r, c).start()

    def z_arrived(j):
        pltpu.make_async_remote_copy(
            src_ref=sbuf.at[0], dst_ref=xg.at[mt, j],
            send_sem=z_send.at[j], recv_sem=z_recv.at[j],
            device_id={"ep": me}, device_id_type=MESH,
        ).wait_recv()

    def gather_first(c, skip):
        for k in range(skip, SLOTS):
            z_arrived(c * SLOTS + k)
        for d in range(2):
            ag_start(d, 0, c)

    def gather_next(s, c):
        for d in range(2):
            ag_wait(d, s - 1, c)
            ag_start(d, s, c)

    def finish(c):
        for d in range(2):
            rs_copy(d, hops - 1, c).wait_recv()
        y = (
            part[c, mt]
            + rs[0, hops - 1, c].astype(F32)
            + rs[1, hops - 1, c].astype(F32)
        ).astype(BF16)
        yout[pl.ds(c * SLOTS, SLOTS)] = y.reshape(SLOTS, 2 * cap, 128)
        for cc in range(chunks):

            @pl.when(c == cc)
            def _():
                for k in range(SLOTS):
                    if cc or k:
                        ret_copy(cc * SLOTS + k).start()

    def computed(t, delay, f):
        first = t - hops - delay

        @pl.when((first >= 0) & (first < chunks - 1))
        def _():
            pl.loop(first, first + 1 + (first + 1) // (chunks - 1))(f)

    @pl.loop(0, chunks - 1 + 2 * hops)
    def _(t):
        @pl.when(t == hops)
        def _():
            for load in loads:
                load.wait()

        @functools.partial(computed, t, 0)
        def _(c):
            for d in range(2):
                ag_wait(d, hops - 1, c)
            compute(c)
            for d in range(2):
                reduce_step(d, 0, c)

        for s in range(hops - 1, 0, -1):

            @pl.when(t == s)
            def _():
                gather_next(s, 0)

            @pl.when((t - s + 1 >= 1) & (t - s + 1 < chunks))
            def _():
                gather_next(s, t - s + 1)

        @pl.when(t == 0)
        def _():
            gather_first(0, 1)

        @pl.when(t + 1 < chunks)
        def _():
            gather_first(t + 1, 0)

        pl.when(t == 0)(combine_weights)

        for r in range(1, hops):

            @functools.partial(computed, t, r)
            def _(c):
                for d in range(2):
                    reduce_step(d, r, c)

        computed(t, hops, finish)

    back[0] = yout[0]
    mixed = jnp.zeros((tok_count, feats), F32)
    for g in range(groups):

        for j in range(max(1, g * wide), (g + 1) * wide):
            ret_copy(j).wait_recv()

        b4 = back[g * wide : (g + 1) * wide].reshape(2 * grows, 128).astype(F32)
        b4 = b4.reshape(grows // 8, 2, 8, 128)
        left = b4[:, 0].reshape(grows, 128).astype(BF16)
        right = b4[:, 1].reshape(grows, 128).astype(BF16)
        picked = jnp.concatenate([left, right], axis=1)
        mixed = mixed + dot_nn(wt[g, 0], picked) + dot_nn(wt[g, 1], picked)
    out_ref[...] = mixed.astype(BF16)

    for j in range(1, n_ep):
        z_copy(j).wait_send()
        ret_copy(j).wait_send()

    @pl.loop(0, chunks)
    def _(c):
        for d in range(2):
            for s in range(hops):
                ag_copy(d, s, c, mt).wait_send()
                rs_copy(d, s, c).wait_send()


def on_device(n_ep, n_tp, tokens, norm_gain, expert_ids, gate_weights, w_gate, w_up, w_down):
    tok_count, feats = tokens.shape
    cap = 3 * tok_count * expert_ids.shape[1] // (2 * n_ep)
    width, ff = w_gate.shape[1:]
    chunks, hops = n_ep // SLOTS, n_tp // 2
    rows = SLOTS * cap
    vmem = pl.BlockSpec(memory_space=pltpu.VMEM)
    hbm = pl.BlockSpec(memory_space=pl.ANY)
    dma = pltpu.SemaphoreType.DMA
    block = (n_ep, 2 * cap, 128)
    return pl.pallas_call(
        functools.partial(kernel, n_ep, n_tp, cap),
        out_shape=jax.ShapeDtypeStruct((tok_count, feats), BF16),
        in_specs=[hbm] * 7,
        out_specs=vmem,
        scratch_shapes=[
            pltpu.VMEM((tok_count, feats), BF16),
            pltpu.VMEM((width // 128, 128), F32),
            pltpu.VMEM((2, tok_count), jnp.int32),
            pltpu.VMEM((2, tok_count), F32),
            pltpu.VMEM((width, 2 * ff), BF16),
            pltpu.VMEM((ff, width), BF16),
            pltpu.VMEM(block, BF16),
            pltpu.VMEM((n_tp, *block), BF16),
            pltpu.VMEM((rows, width), BF16),
            pltpu.VMEM((chunks, n_tp, 2 * rows, 128), F32),
            pltpu.VMEM((2, hops, chunks, 2 * rows, 128), BF16),
            pltpu.VMEM((2, hops, chunks, 2 * rows, 128), BF16),
            pltpu.VMEM(block, BF16),
            pltpu.VMEM(block, BF16),
            pltpu.VMEM((chunks // GROUP, 2, tok_count, GROUP * rows), BF16),
            dma((4,)),
            dma((3,)),
            dma((n_ep,)),
            dma((n_ep,)),
            dma((2, hops, chunks)),
            dma((2, hops, chunks)),
            dma((2, hops, chunks)),
            dma((2, hops, chunks)),
            dma((n_ep,)),
            dma((n_ep,)),
        ],
        compiler_params=pltpu.CompilerParams(
            collective_id=0, has_side_effects=True
        ),
    )(
        tokens,
        norm_gain.reshape(-1, 128),
        expert_ids.T,
        gate_weights.T,
        w_gate[0],
        w_up[0],
        w_down[0],
    )


def solution(mesh):
    rows = ("grp", "ep")
    return jax.shard_map(
        functools.partial(on_device, mesh.shape["ep"], mesh.shape["tp"]),
        mesh=mesh,
        in_specs=(
            P(rows, "tp"),
            P(),
            P(rows, None),
            P(rows, None),
            P("ep", None, "tp"),
            P("ep", None, "tp"),
            P("ep", "tp", None),
        ),
        out_specs=P(rows, "tp"),
        check_vma=False,
    )
```

```python
import functools

import jax
import jax.numpy as jnp
from jax import lax
from jax.experimental import pallas as pl
from jax.experimental.pallas import tpu as pltpu
from jax.sharding import PartitionSpec as P

MESH = pl.DeviceIdType.MESH
F32 = jnp.float32
BF16 = jnp.bfloat16
EPS = 1e-06
SLOTS = 4
GROUP = 2
STEPS = (0, 1, 4, -4, 5, -5, 6, -6, 7, -7, 8, 3, -3, 2, -2, -1)


def steps_of(n_z):
    if n_z == len(STEPS):
        return list(STEPS)
    return [0] + [(i + 1) // 2 * (1 if i % 2 else -1) for i in range(1, n_z)]


def dot_nn(a, b):
    return jnp.dot(a, b, preferred_element_type=F32)


def dot_nt(a, b):
    return lax.dot_general(a, b, (((1,), (1,)), ((), ())), preferred_element_type=F32)


def stacked(y):
    rows = y.shape[0]
    left = y[:, :128].reshape(rows // 8, 1, 8, 128)
    right = y[:, 128:].reshape(rows // 8, 1, 8, 128)
    return jnp.concatenate([left, right], axis=1).reshape(2 * rows, 128)


def kernel(
    n_ep, n_tp, cap,
    tok_hbm, gain_hbm, ids_hbm, gw_hbm, wg_ref, wu_ref, wd_ref,
    out_ref,
    tok_ref, gain_ref, ids_ref, gw_ref,
    wgu, wdn, sbuf, xg, lhs, part, stage, rs, yout, back, wt,
    in_sem, w_sem, z_send, z_recv, ag_send, ag_recv, rs_send, rs_recv, ret_send, ret_recv,
):
    n_z = n_ep // 2
    hops = n_tp // 2
    chunks = n_ep // SLOTS
    groups = chunks // GROUP
    wide = GROUP * SLOTS
    tok_count, feats = tok_ref.shape
    ff = wg_ref.shape[1]
    width = feats * n_tp
    rows = SLOTS * cap
    rows2 = 2 * rows
    grows = wide * cap
    half = SLOTS // 2
    me = lax.axis_index("ep")
    mt = lax.axis_index("tp")
    z, core = me // 2, me % 2
    SGN = (1, -1)

    ins = [
        pltpu.make_async_copy(ids_hbm, ids_ref, in_sem.at[0]),
        pltpu.make_async_copy(tok_hbm, tok_ref, in_sem.at[1]),
        pltpu.make_async_copy(gw_hbm, gw_ref, in_sem.at[2]),
        pltpu.make_async_copy(gain_hbm, gain_ref, in_sem.at[3]),
    ]
    for load in ins:
        load.start()

    barrier = pltpu.get_barrier_semaphore()

    @pl.loop(0, n_ep - 1)
    def _(i):
        d = n_ep // 2 + ((i + 1) // 2) * (1 - 2 * (i % 2))
        pl.semaphore_signal(
            barrier, inc=1, device_id={"ep": (me + d) % n_ep}, device_id_type=MESH
        )

    for sg in SGN:
        pl.semaphore_signal(
            barrier, inc=1, device_id={"tp": (mt + sg + n_tp) % n_tp}, device_id_type=MESH
        )

    loads = [
        pltpu.make_async_copy(wg_ref, wgu.at[:, pl.ds(0, ff)], w_sem.at[0]),
        pltpu.make_async_copy(wu_ref, wgu.at[:, pl.ds(ff, ff)], w_sem.at[1]),
        pltpu.make_async_copy(wd_ref, wdn, w_sem.at[2]),
    ]
    for load in loads:
        load.start()

    steps = steps_of(n_z)

    def peer(j, sign):
        zz = (z + sign * steps[j // 2] + n_z) % n_z
        return zz * 2 + (core + j % 2) % 2

    for load in ins:
        load.wait()
    j_iota = lax.broadcasted_iota(jnp.int32, (n_ep, 1), 0)
    e_iota = jnp.zeros((n_ep, 1), jnp.int32)
    for j in range(n_ep):
        e_iota = jnp.where(j_iota == j, peer(j, -1), e_iota)
    m0 = ids_ref[0:1, :] == e_iota
    m1 = ids_ref[1:2, :] == e_iota
    member = jnp.where(m0 | m1, 1.0, 0.0).astype(F32)
    member_b = member.astype(BF16)
    t_row = lax.broadcasted_iota(jnp.int32, (tok_count, tok_count), 0)
    t_col = lax.broadcasted_iota(jnp.int32, (tok_count, tok_count), 1)
    upper = jnp.where(t_row < t_col, 1.0, 0.0).astype(BF16)
    rank = dot_nn(member_b, upper)
    rank = jnp.where(member > 0.5, rank, -1.0).astype(BF16)
    x_row = lax.broadcasted_iota(jnp.int32, (wide, cap, n_ep), 0)
    x_col = lax.broadcasted_iota(jnp.int32, (wide, cap, n_ep), 2)
    c_iota = lax.broadcasted_iota(jnp.int32, (wide, cap, tok_count), 1).astype(F32)
    c_iota = c_iota.reshape(grows, tok_count)

    def z_copy(j):
        return pltpu.make_async_remote_copy(
            src_ref=sbuf.at[j], dst_ref=xg.at[mt, j],
            send_sem=z_send, recv_sem=z_recv.at[j // SLOTS],
            device_id={"ep": peer(j, -1)}, device_id_type=MESH,
        )

    def ret_copy(j):
        return pltpu.make_async_remote_copy(
            src_ref=yout.at[j], dst_ref=back.at[j],
            send_sem=ret_send, recv_sem=ret_recv.at[j // wide],
            device_id={"ep": peer(j, 1)}, device_id_type=MESH,
        )

    for g in range(groups):
        expand = jnp.where(x_row + g * wide == x_col, 1.0, 0.0).astype(F32)
        expand = expand.reshape(grows, n_ep).astype(BF16)
        pick = jnp.where(dot_nn(expand, rank) == c_iota, 1.0, 0.0).astype(BF16)
        sent = stacked(dot_nn(pick, tok_ref[...])).astype(BF16)
        sbuf[g * wide : (g + 1) * wide] = sent.reshape(wide, 2 * cap, 128)
        if g == 0:
            xg[mt, 0] = sbuf[0]
            pl.semaphore_wait(barrier, n_ep - 1 + 2)

        for j in range(max(1, g * wide), (g + 1) * wide):
            z_copy(j).start()

    def ag_copy(d, s, c, block):
        start = c * SLOTS
        count = SLOTS
        if s == hops - 1:
            start = start + (0 if d == 0 else half)
            count = half
        ref = xg.at[block, pl.ds(start, count)]
        return pltpu.make_async_remote_copy(
            src_ref=ref, dst_ref=ref,
            send_sem=ag_send, recv_sem=ag_recv.at[d, s, c],
            device_id={"tp": (mt + SGN[d] + n_tp) % n_tp}, device_id_type=MESH,
        )

    def ag_start(d, s, c):
        ag_copy(d, s, c, (mt - SGN[d] * s + n_tp) % n_tp).start()

    def ag_wait(d, s, c):
        ag_copy(d, s, c, (mt - SGN[d] * (s + 1) + n_tp) % n_tp).wait_recv()

    def rs_copy(d, r, c):
        if r == 0:
            span = pl.ds(0 if d == 0 else rows, rows)
            src, dst = stage.at[d, r, c, span], rs.at[d, r, c, span]
        else:
            src, dst = stage.at[d, r, c], rs.at[d, r, c]
        return pltpu.make_async_remote_copy(
            src_ref=src, dst_ref=dst,
            send_sem=rs_send, recv_sem=rs_recv.at[d, r, c],
            device_id={"tp": (mt + SGN[d] + n_tp) % n_tp}, device_id_type=MESH,
        )

    def combine_weights():
        eye = jnp.where(t_row == t_col, 1.0, 0.0).astype(BF16)
        lower = jnp.where(t_col < t_row, 1.0, 0.0).astype(BF16)
        gate_w = jnp.where(m0, gw_ref[0:1, :], 0.0) + jnp.where(m1, gw_ref[1:2, :], 0.0)
        gate_hi = gate_w.astype(BF16)
        gate_lo = (gate_w - gate_hi.astype(F32)).astype(BF16)
        rank_t = jnp.where(dot_nt(eye, member_b) > 0.5, dot_nt(lower, member_b), -1.0)
        rank_t = rank_t.astype(BF16)
        hi_t = dot_nt(eye, gate_hi).astype(BF16)
        lo_t = dot_nt(eye, gate_lo).astype(BF16)
        l_e = lax.broadcasted_iota(jnp.int32, (n_ep, grows), 0) * cap
        l_s = lax.broadcasted_iota(jnp.int32, (n_ep, grows), 1)
        lane = lax.broadcasted_iota(jnp.int32, (tok_count, grows), 1).astype(F32)
        lane = lane - cap * jnp.floor((lane + 0.5) * (1.0 / cap))
        for g in range(groups):
            s = l_s + g * grows
            expand_t = jnp.where((s >= l_e) & (s < l_e + cap), 1.0, 0.0).astype(BF16)
            hit = dot_nn(rank_t, expand_t) == lane
            wt[g, 0] = jnp.where(hit, dot_nn(hi_t, expand_t), 0.0).astype(BF16)
            wt[g, 1] = jnp.where(hit, dot_nn(lo_t, expand_t), 0.0).astype(BF16)

    def compute(c):
        total = jnp.zeros((rows // 8, 8, 128), F32)
        for b in range(n_tp):
            v = xg[b, pl.ds(c * SLOTS, SLOTS)].reshape(rows2, 128).astype(F32)
            v = v.reshape(rows // 8, 2, 8, 128)
            for h in range(2):
                vh = v[:, h]
                total = total + vh * vh
                k = 2 * b + h
                scaled = vh * gain_ref[k : k + 1, :].reshape(1, 1, 128)
                lhs[:, k * 128 : (k + 1) * 128] = scaled.reshape(rows, 128).astype(BF16)
        square = jnp.sum(total.reshape(rows, 128), axis=1, keepdims=True)
        scale = lax.rsqrt(square / width + EPS)
        gu = dot_nn(lhs[...], wgu[...])
        gate = gu[:, :ff] * scale
        up = gu[:, ff:] * scale
        hidden = (gate / (1.0 + jnp.exp(-gate)) * up).astype(BF16)
        y = dot_nn(hidden, wdn[...])
        for b in range(n_tp):
            part[c, b] = stacked(y[:, b * feats : (b + 1) * feats])

    def reduce_step(d, r, c):
        block = (mt + SGN[d] * (hops - r) + n_tp) % n_tp
        own = slice(0, rows) if d == 0 else slice(rows, rows2)
        rest = slice(rows, rows2) if d == 0 else slice(0, rows)
        if r == 0:
            stage[d, r, c, own] = part[c, block, own].astype(BF16)
        elif r == 1:
            rs_copy(d, 0, c).wait_recv()
            stage[d, r, c, own] = (
                part[c, block, own] + rs[d, 0, c, own].astype(F32)
            ).astype(BF16)
            stage[d, r, c, rest] = part[c, block, rest].astype(BF16)
        else:
            rs_copy(d, r - 1, c).wait_recv()
            stage[d, r, c] = (part[c, block] + rs[d, r - 1, c].astype(F32)).astype(BF16)
        rs_copy(d, r, c).start()

    def bytes_of(ref, send_sem, recv_sem):
        return pltpu.make_async_remote_copy(
            src_ref=ref, dst_ref=ref, send_sem=send_sem, recv_sem=recv_sem,
            device_id={"ep": me}, device_id_type=MESH,
        )

    def gather_first(c, skip):
        slots = pl.ds(c * SLOTS + skip, SLOTS - skip)
        bytes_of(xg.at[mt, slots], z_send, z_recv.at[c]).wait_recv()
        for d in range(2):
            ag_start(d, 0, c)

    def gather_next(s, c):
        for d in range(2):
            ag_wait(d, s - 1, c)
            ag_start(d, s, c)

    def finish(c):
        for d in range(2):
            rs_copy(d, hops - 1, c).wait_recv()
        y = (
            part[c, mt]
            + rs[0, hops - 1, c].astype(F32)
            + rs[1, hops - 1, c].astype(F32)
        ).astype(BF16)
        yout[pl.ds(c * SLOTS, SLOTS)] = y.reshape(SLOTS, 2 * cap, 128)
        for cc in range(chunks):

            @pl.when(c == cc)
            def _():
                for k in range(SLOTS):
                    if cc or k:
                        ret_copy(cc * SLOTS + k).start()

    def computed(t, delay, f):
        first = t - hops - delay

        @pl.when((first >= 0) & (first < chunks - 1))
        def _():
            pl.loop(first, first + 1 + (first + 1) // (chunks - 1))(f)

    @pl.loop(0, chunks - 1 + 2 * hops)
    def _(t):
        @pl.when(t == hops)
        def _():
            for load in loads:
                load.wait()

        @functools.partial(computed, t, 0)
        def _(c):
            for d in range(2):
                ag_wait(d, hops - 1, c)
            compute(c)
            for d in range(2):
                reduce_step(d, 0, c)

        for s in range(hops - 1, 0, -1):

            @pl.when(t == s)
            def _():
                gather_next(s, 0)

            @pl.when((t - s + 1 >= 1) & (t - s + 1 < chunks))
            def _():
                gather_next(s, t - s + 1)

        @pl.when(t == 0)
        def _():
            gather_first(0, 1)

        @pl.when(t + 1 < chunks)
        def _():
            gather_first(t + 1, 0)

        pl.when(t == 0)(combine_weights)

        for r in range(1, hops):

            @functools.partial(computed, t, r)
            def _(c):
                for d in range(2):
                    reduce_step(d, r, c)

        computed(t, hops, finish)

    others = pl.ds(1, n_ep - 1)
    blocks = xg.at[pl.ds(0, n_tp - 1)]
    bytes_of(sbuf.at[others], z_send, z_recv.at[0]).wait_send()
    bytes_of(blocks, ag_send, z_recv.at[0]).wait_send()
    bytes_of(blocks, rs_send, z_recv.at[0]).wait_send()

    back[0] = yout[0]
    mixed = jnp.zeros((tok_count, feats), F32)
    for g in range(groups):

        first = max(1, g * wide)
        arrived = back.at[pl.ds(first, (g + 1) * wide - first)]
        bytes_of(arrived, ret_send, ret_recv.at[g]).wait_recv()

        b4 = back[g * wide : (g + 1) * wide].reshape(2 * grows, 128).astype(F32)
        b4 = b4.reshape(grows // 8, 2, 8, 128)
        left = b4[:, 0].reshape(grows, 128).astype(BF16)
        right = b4[:, 1].reshape(grows, 128).astype(BF16)
        picked = jnp.concatenate([left, right], axis=1)
        mixed = mixed + dot_nn(wt[g, 0], picked) + dot_nn(wt[g, 1], picked)
    out_ref[...] = mixed.astype(BF16)

    bytes_of(yout.at[others], ret_send, ret_recv.at[0]).wait_send()


def on_device(n_ep, n_tp, tokens, norm_gain, expert_ids, gate_weights, w_gate, w_up, w_down):
    tok_count, feats = tokens.shape
    cap = 3 * tok_count * expert_ids.shape[1] // (2 * n_ep)
    width, ff = w_gate.shape[1:]
    chunks, hops = n_ep // SLOTS, n_tp // 2
    rows = SLOTS * cap
    vmem = pl.BlockSpec(memory_space=pltpu.VMEM)
    hbm = pl.BlockSpec(memory_space=pl.ANY)
    dma = pltpu.SemaphoreType.DMA
    block = (n_ep, 2 * cap, 128)
    return pl.pallas_call(
        functools.partial(kernel, n_ep, n_tp, cap),
        out_shape=jax.ShapeDtypeStruct((tok_count, feats), BF16),
        in_specs=[hbm] * 7,
        out_specs=vmem,
        scratch_shapes=[
            pltpu.VMEM((tok_count, feats), BF16),
            pltpu.VMEM((width // 128, 128), F32),
            pltpu.VMEM((2, tok_count), jnp.int32),
            pltpu.VMEM((2, tok_count), F32),
            pltpu.VMEM((width, 2 * ff), BF16),
            pltpu.VMEM((ff, width), BF16),
            pltpu.VMEM(block, BF16),
            pltpu.VMEM((n_tp, *block), BF16),
            pltpu.VMEM((rows, width), BF16),
            pltpu.VMEM((chunks, n_tp, 2 * rows, 128), F32),
            pltpu.VMEM((2, hops, chunks, 2 * rows, 128), BF16),
            pltpu.VMEM((2, hops, chunks, 2 * rows, 128), BF16),
            pltpu.VMEM(block, BF16),
            pltpu.VMEM(block, BF16),
            pltpu.VMEM((chunks // GROUP, 2, tok_count, GROUP * rows), BF16),
            dma((4,)),
            dma((3,)),
            dma,
            dma((chunks,)),
            dma,
            dma((2, hops, chunks)),
            dma,
            dma((2, hops, chunks)),
            dma,
            dma((chunks // GROUP,)),
        ],
        compiler_params=pltpu.CompilerParams(
            collective_id=0, has_side_effects=True
        ),
    )(
        tokens,
        norm_gain.reshape(-1, 128),
        expert_ids.T,
        gate_weights.T,
        w_gate[0],
        w_up[0],
        w_down[0],
    )


def solution(mesh):
    rows = ("grp", "ep")
    return jax.shard_map(
        functools.partial(on_device, mesh.shape["ep"], mesh.shape["tp"]),
        mesh=mesh,
        in_specs=(
            P(rows, "tp"),
            P(),
            P(rows, None),
            P(rows, None),
            P("ep", None, "tp"),
            P("ep", None, "tp"),
            P("ep", "tp", None),
        ),
        out_specs=P(rows, "tp"),
        check_vma=False,
    )
```

```python
import functools

import jax
import jax.numpy as jnp
from jax import lax
from jax.experimental import pallas as pl
from jax.experimental.pallas import tpu as pltpu
from jax.sharding import PartitionSpec as P

MESH = pl.DeviceIdType.MESH
F32 = jnp.float32
BF16 = jnp.bfloat16
EPS = 1e-06
SLOTS = 4
GROUP = 2
STEPS = (0, 1, 3, -4, 5, -5, 6, -6, 8, -7, 7, 4, -3, 2, -2, -1)


def steps_of(n_z):
    if n_z == len(STEPS):
        return list(STEPS)
    return [0] + [(i + 1) // 2 * (1 if i % 2 else -1) for i in range(1, n_z)]


def dot_nn(a, b):
    return jnp.dot(a, b, preferred_element_type=F32)


def dot_nt(a, b):
    return lax.dot_general(a, b, (((1,), (1,)), ((), ())), preferred_element_type=F32)


def stacked(y):
    rows = y.shape[0]
    left = y[:, :128].reshape(rows // 8, 1, 8, 128)
    right = y[:, 128:].reshape(rows // 8, 1, 8, 128)
    return jnp.concatenate([left, right], axis=1).reshape(2 * rows, 128)


def kernel(
    n_ep, n_tp, cap,
    tok_hbm, gain_hbm, ids_hbm, gw_hbm, wg_ref, wu_ref, wd_ref,
    out_ref,
    tok_ref, gain_ref, ids_ref, gw_ref,
    wgu, wdn, sbuf, xg, lhs, part, stage, rs, yout, back, wt,
    in_sem, w_sem, z_send, z_recv, ag_send, ag_recv, rs_send, rs_recv, ret_send, ret_recv,
):
    n_z = n_ep // 2
    hops = n_tp // 2
    chunks = n_ep // SLOTS
    groups = chunks // GROUP
    wide = GROUP * SLOTS
    tok_count, feats = tok_ref.shape
    ff = wg_ref.shape[1]
    width = feats * n_tp
    rows = SLOTS * cap
    rows2 = 2 * rows
    grows = wide * cap
    half = SLOTS // 2
    me = lax.axis_index("ep")
    mt = lax.axis_index("tp")
    z, core = me // 2, me % 2
    SGN = (1, -1)

    ins = [
        pltpu.make_async_copy(ids_hbm, ids_ref, in_sem.at[0]),
        pltpu.make_async_copy(tok_hbm, tok_ref, in_sem.at[1]),
        pltpu.make_async_copy(gw_hbm, gw_ref, in_sem.at[2]),
        pltpu.make_async_copy(gain_hbm, gain_ref, in_sem.at[3]),
    ]
    for load in ins:
        load.start()

    barrier = pltpu.get_barrier_semaphore()

    @pl.loop(0, n_ep - 1)
    def _(i):
        d = n_ep // 2 + ((i + 1) // 2) * (1 - 2 * (i % 2))
        pl.semaphore_signal(
            barrier, inc=1, device_id={"ep": (me + d) % n_ep}, device_id_type=MESH
        )

    for sg in SGN:
        pl.semaphore_signal(
            barrier, inc=1, device_id={"tp": (mt + sg + n_tp) % n_tp}, device_id_type=MESH
        )

    loads = [
        pltpu.make_async_copy(wg_ref, wgu.at[:, pl.ds(0, ff)], w_sem.at[0]),
        pltpu.make_async_copy(wu_ref, wgu.at[:, pl.ds(ff, ff)], w_sem.at[1]),
        pltpu.make_async_copy(wd_ref, wdn, w_sem.at[2]),
    ]
    for load in loads:
        load.start()

    steps = steps_of(n_z)

    def peer(j, sign):
        zz = (z + sign * steps[j // 2] + n_z) % n_z
        return zz * 2 + (core + j % 2) % 2

    for load in ins:
        load.wait()
    j_iota = lax.broadcasted_iota(jnp.int32, (n_ep, 1), 0)
    e_iota = jnp.zeros((n_ep, 1), jnp.int32)
    for j in range(n_ep):
        e_iota = jnp.where(j_iota == j, peer(j, -1), e_iota)
    m0 = ids_ref[0:1, :] == e_iota
    m1 = ids_ref[1:2, :] == e_iota
    member = jnp.where(m0 | m1, 1.0, 0.0).astype(F32)
    member_b = member.astype(BF16)
    t_row = lax.broadcasted_iota(jnp.int32, (tok_count, tok_count), 0)
    t_col = lax.broadcasted_iota(jnp.int32, (tok_count, tok_count), 1)
    upper = jnp.where(t_row < t_col, 1.0, 0.0).astype(BF16)
    rank = dot_nn(member_b, upper)
    rank = jnp.where(member > 0.5, rank, -1.0).astype(BF16)
    x_row = lax.broadcasted_iota(jnp.int32, (wide, cap, n_ep), 0)
    x_col = lax.broadcasted_iota(jnp.int32, (wide, cap, n_ep), 2)
    c_iota = lax.broadcasted_iota(jnp.int32, (wide, cap, tok_count), 1).astype(F32)
    c_iota = c_iota.reshape(grows, tok_count)

    def z_copy(j):
        return pltpu.make_async_remote_copy(
            src_ref=sbuf.at[j], dst_ref=xg.at[mt, j],
            send_sem=z_send, recv_sem=z_recv.at[j // SLOTS],
            device_id={"ep": peer(j, -1)}, device_id_type=MESH,
        )

    def ret_copy(j):
        return pltpu.make_async_remote_copy(
            src_ref=yout.at[j], dst_ref=back.at[j],
            send_sem=ret_send, recv_sem=ret_recv.at[j // wide],
            device_id={"ep": peer(j, 1)}, device_id_type=MESH,
        )

    for g in range(groups):
        expand = jnp.where(x_row + g * wide == x_col, 1.0, 0.0).astype(F32)
        expand = expand.reshape(grows, n_ep).astype(BF16)
        pick = jnp.where(dot_nn(expand, rank) == c_iota, 1.0, 0.0).astype(BF16)
        sent = stacked(dot_nn(pick, tok_ref[...])).astype(BF16)
        sbuf[g * wide : (g + 1) * wide] = sent.reshape(wide, 2 * cap, 128)
        if g == 0:
            xg[mt, 0] = sbuf[0]
            pl.semaphore_wait(barrier, n_ep - 1 + 2)

        for j in range(max(1, g * wide), (g + 1) * wide):
            z_copy(j).start()

    def ag_copy(d, s, c, block):
        start = c * SLOTS
        count = SLOTS
        if s == hops - 1:
            start = start + (0 if d == 0 else half)
            count = half
        ref = xg.at[block, pl.ds(start, count)]
        return pltpu.make_async_remote_copy(
            src_ref=ref, dst_ref=ref,
            send_sem=ag_send, recv_sem=ag_recv.at[d, s, c],
            device_id={"tp": (mt + SGN[d] + n_tp) % n_tp}, device_id_type=MESH,
        )

    def ag_start(d, s, c):
        ag_copy(d, s, c, (mt - SGN[d] * s + n_tp) % n_tp).start()

    def ag_wait(d, s, c):
        ag_copy(d, s, c, (mt - SGN[d] * (s + 1) + n_tp) % n_tp).wait_recv()

    def rs_copy(d, r, c):
        if r == 0:
            span = pl.ds(0 if d == 0 else rows, rows)
            src, dst = stage.at[d, r, c, span], rs.at[d, r, c, span]
        else:
            src, dst = stage.at[d, r, c], rs.at[d, r, c]
        return pltpu.make_async_remote_copy(
            src_ref=src, dst_ref=dst,
            send_sem=rs_send, recv_sem=rs_recv.at[d, r, c],
            device_id={"tp": (mt + SGN[d] + n_tp) % n_tp}, device_id_type=MESH,
        )

    def combine_weights():
        eye = jnp.where(t_row == t_col, 1.0, 0.0).astype(BF16)
        lower = jnp.where(t_col < t_row, 1.0, 0.0).astype(BF16)
        gate_w = jnp.where(m0, gw_ref[0:1, :], 0.0) + jnp.where(m1, gw_ref[1:2, :], 0.0)
        gate_hi = gate_w.astype(BF16)
        gate_lo = (gate_w - gate_hi.astype(F32)).astype(BF16)
        rank_t = jnp.where(dot_nt(eye, member_b) > 0.5, dot_nt(lower, member_b), -1.0)
        rank_t = rank_t.astype(BF16)
        hi_t = dot_nt(eye, gate_hi).astype(BF16)
        lo_t = dot_nt(eye, gate_lo).astype(BF16)
        l_e = lax.broadcasted_iota(jnp.int32, (n_ep, grows), 0) * cap
        l_s = lax.broadcasted_iota(jnp.int32, (n_ep, grows), 1)
        lane = lax.broadcasted_iota(jnp.int32, (tok_count, grows), 1).astype(F32)
        lane = lane - cap * jnp.floor((lane + 0.5) * (1.0 / cap))
        for g in range(groups):
            s = l_s + g * grows
            expand_t = jnp.where((s >= l_e) & (s < l_e + cap), 1.0, 0.0).astype(BF16)
            hit = dot_nn(rank_t, expand_t) == lane
            wt[g, 0] = jnp.where(hit, dot_nn(hi_t, expand_t), 0.0).astype(BF16)
            wt[g, 1] = jnp.where(hit, dot_nn(lo_t, expand_t), 0.0).astype(BF16)

    def compute(c):
        total = jnp.zeros((rows // 8, 8, 128), F32)
        for b in range(n_tp):
            v = xg[b, pl.ds(c * SLOTS, SLOTS)].reshape(rows2, 128).astype(F32)
            v = v.reshape(rows // 8, 2, 8, 128)
            for h in range(2):
                vh = v[:, h]
                total = total + vh * vh
                k = 2 * b + h
                scaled = vh * gain_ref[k : k + 1, :].reshape(1, 1, 128)
                lhs[:, k * 128 : (k + 1) * 128] = scaled.reshape(rows, 128).astype(BF16)
        square = jnp.sum(total.reshape(rows, 128), axis=1, keepdims=True)
        scale = lax.rsqrt(square / width + EPS)
        gu = dot_nn(lhs[...], wgu[...])
        gate = gu[:, :ff] * scale
        up = gu[:, ff:] * scale
        hidden = (gate / (1.0 + jnp.exp(-gate)) * up).astype(BF16)
        y = dot_nn(hidden, wdn[...])
        for b in range(n_tp):
            part[c, b] = stacked(y[:, b * feats : (b + 1) * feats])

    def reduce_step(d, r, c):
        block = (mt + SGN[d] * (hops - r) + n_tp) % n_tp
        own = slice(0, rows) if d == 0 else slice(rows, rows2)
        rest = slice(rows, rows2) if d == 0 else slice(0, rows)
        if r == 0:
            stage[d, r, c, own] = part[c, block, own].astype(BF16)
        elif r == 1:
            rs_copy(d, 0, c).wait_recv()
            stage[d, r, c, own] = (
                part[c, block, own] + rs[d, 0, c, own].astype(F32)
            ).astype(BF16)
            stage[d, r, c, rest] = part[c, block, rest].astype(BF16)
        else:
            rs_copy(d, r - 1, c).wait_recv()
            stage[d, r, c] = (part[c, block] + rs[d, r - 1, c].astype(F32)).astype(BF16)
        rs_copy(d, r, c).start()

    def bytes_of(ref, send_sem, recv_sem):
        return pltpu.make_async_remote_copy(
            src_ref=ref, dst_ref=ref, send_sem=send_sem, recv_sem=recv_sem,
            device_id={"ep": me}, device_id_type=MESH,
        )

    def gather_first(c, skip):
        slots = pl.ds(c * SLOTS + skip, SLOTS - skip)
        bytes_of(xg.at[mt, slots], z_send, z_recv.at[c]).wait_recv()
        for d in range(2):
            ag_start(d, 0, c)

    def gather_next(s, c):
        for d in range(2):
            ag_wait(d, s - 1, c)
            ag_start(d, s, c)

    def finish(c):
        for d in range(2):
            rs_copy(d, hops - 1, c).wait_recv()
        y = (
            part[c, mt]
            + rs[0, hops - 1, c].astype(F32)
            + rs[1, hops - 1, c].astype(F32)
        ).astype(BF16)
        yout[pl.ds(c * SLOTS, SLOTS)] = y.reshape(SLOTS, 2 * cap, 128)
        for cc in range(chunks):

            @pl.when(c == cc)
            def _():
                for k in range(SLOTS):
                    if cc or k:
                        ret_copy(cc * SLOTS + k).start()

    def computed(t, delay, f):
        first = t - hops - delay

        @pl.when((first >= 0) & (first < chunks - 1))
        def _():
            pl.loop(first, first + 1 + (first + 1) // (chunks - 1))(f)

    @pl.loop(0, chunks - 1 + 2 * hops)
    def _(t):
        @pl.when(t == hops)
        def _():
            for load in loads:
                load.wait()

        @functools.partial(computed, t, 0)
        def _(c):
            for d in range(2):
                ag_wait(d, hops - 1, c)
            compute(c)
            for d in range(2):
                reduce_step(d, 0, c)

        for s in range(hops - 1, 0, -1):

            @pl.when(t == s)
            def _():
                gather_next(s, 0)

            @pl.when((t - s + 1 >= 1) & (t - s + 1 < chunks))
            def _():
                gather_next(s, t - s + 1)

        @pl.when(t == 0)
        def _():
            gather_first(0, 1)

        @pl.when(t + 1 < chunks)
        def _():
            gather_first(t + 1, 0)

        pl.when(t == 0)(combine_weights)

        for r in range(1, hops):

            @functools.partial(computed, t, r)
            def _(c):
                for d in range(2):
                    reduce_step(d, r, c)

        computed(t, hops, finish)

    others = pl.ds(1, n_ep - 1)
    blocks = xg.at[pl.ds(0, n_tp - 1)]
    bytes_of(sbuf.at[others], z_send, z_recv.at[0]).wait_send()
    bytes_of(blocks, ag_send, z_recv.at[0]).wait_send()
    bytes_of(blocks, rs_send, z_recv.at[0]).wait_send()

    back[0] = yout[0]
    mixed = jnp.zeros((tok_count, feats), F32)
    for g in range(groups):

        first = max(1, g * wide)
        arrived = back.at[pl.ds(first, (g + 1) * wide - first)]
        bytes_of(arrived, ret_send, ret_recv.at[g]).wait_recv()

        b4 = back[g * wide : (g + 1) * wide].reshape(2 * grows, 128).astype(F32)
        b4 = b4.reshape(grows // 8, 2, 8, 128)
        left = b4[:, 0].reshape(grows, 128).astype(BF16)
        right = b4[:, 1].reshape(grows, 128).astype(BF16)
        picked = jnp.concatenate([left, right], axis=1)
        mixed = mixed + dot_nn(wt[g, 0], picked) + dot_nn(wt[g, 1], picked)
    out_ref[...] = mixed.astype(BF16)

    bytes_of(yout.at[others], ret_send, ret_recv.at[0]).wait_send()


def on_device(n_ep, n_tp, tokens, norm_gain, expert_ids, gate_weights, w_gate, w_up, w_down):
    tok_count, feats = tokens.shape
    cap = 3 * tok_count * expert_ids.shape[1] // (2 * n_ep)
    width, ff = w_gate.shape[1:]
    chunks, hops = n_ep // SLOTS, n_tp // 2
    rows = SLOTS * cap
    vmem = pl.BlockSpec(memory_space=pltpu.VMEM)
    hbm = pl.BlockSpec(memory_space=pl.ANY)
    dma = pltpu.SemaphoreType.DMA
    block = (n_ep, 2 * cap, 128)
    return pl.pallas_call(
        functools.partial(kernel, n_ep, n_tp, cap),
        out_shape=jax.ShapeDtypeStruct((tok_count, feats), BF16),
        in_specs=[hbm] * 7,
        out_specs=vmem,
        scratch_shapes=[
            pltpu.VMEM((tok_count, feats), BF16),
            pltpu.VMEM((width // 128, 128), F32),
            pltpu.VMEM((2, tok_count), jnp.int32),
            pltpu.VMEM((2, tok_count), F32),
            pltpu.VMEM((width, 2 * ff), BF16),
            pltpu.VMEM((ff, width), BF16),
            pltpu.VMEM(block, BF16),
            pltpu.VMEM((n_tp, *block), BF16),
            pltpu.VMEM((rows, width), BF16),
            pltpu.VMEM((chunks, n_tp, 2 * rows, 128), F32),
            pltpu.VMEM((2, hops, chunks, 2 * rows, 128), BF16),
            pltpu.VMEM((2, hops, chunks, 2 * rows, 128), BF16),
            pltpu.VMEM(block, BF16),
            pltpu.VMEM(block, BF16),
            pltpu.VMEM((chunks // GROUP, 2, tok_count, GROUP * rows), BF16),
            dma((4,)),
            dma((3,)),
            dma,
            dma((chunks,)),
            dma,
            dma((2, hops, chunks)),
            dma,
            dma((2, hops, chunks)),
            dma,
            dma((chunks // GROUP,)),
        ],
        compiler_params=pltpu.CompilerParams(
            collective_id=0, has_side_effects=True
        ),
    )(
        tokens,
        norm_gain.reshape(-1, 128),
        expert_ids.T,
        gate_weights.T,
        w_gate[0],
        w_up[0],
        w_down[0],
    )


def solution(mesh):
    rows = ("grp", "ep")
    return jax.shard_map(
        functools.partial(on_device, mesh.shape["ep"], mesh.shape["tp"]),
        mesh=mesh,
        in_specs=(
            P(rows, "tp"),
            P(),
            P(rows, None),
            P(rows, None),
            P("ep", None, "tp"),
            P("ep", None, "tp"),
            P("ep", "tp", None),
        ),
        out_specs=P(rows, "tp"),
        check_vma=False,
    )
```
